32 devices in a mesh: sp: 16 (over z, y, core), tp: 2 (over x).
Axes of the slice: x: 2, y: 2, z: 4, core: 2. Of those that a mesh axis runs over, the one named last changes fastest.
Arguments:
- resid: bfloat16 [8192, 2048], P(('sp', 'tp')), may hold values from -3 to 3
- queries: bfloat16 [8192, 1024], P('sp', 'tp'), may hold values from -6 to 6
- keys: bfloat16 [8192, 512], P('sp', 'tp'), may hold values from -6 to 6
- values: bfloat16 [8192, 512], P('sp', 'tp'), may hold values from -6 to 6
- documents: int32 [8192], P('sp'), may hold values from 0 to 7, never falling along the last dimension, each value on 1 to 2048 neighbouring positions
- sinks: float32 [16], P('tp'), may hold values from 0 to 5
- out_proj: bfloat16 [1024, 2048], replicated, may hold values from -0.75 to 0.75
- norm_gain: float32 [2048], replicated, may hold values from 0.1 to 1.9
- gate_proj: bfloat16 [2048, 5632], P('sp', 'tp'), may hold values from -0.125 to 0.125
- up_proj: bfloat16 [2048, 5632], P('sp', 'tp'), may hold values from -0.125 to 0.125
- down_proj: bfloat16 [5632, 2048], P('tp', 'sp'), may hold values from -0.078125 to 0.078125
Outputs:
- mixed: bfloat16 [8192, 2048], P(('sp', 'tp'))
The draws below stay inside these ranges and needn't reach their ends.
Inputs may be any that keep to these rules, and one draw needn't show every extreme that they name: `documents`: document numbers never fall along the sequence; each document holds at most 2048 positions.
All inputs are finite; a program needn't handle non-finite values.
Results may differ from the reference program's by a relative error of at most 0.0095.
Values may be sent and summed in bfloat16 or wider, within the bound.
No kernel may reach another device: no remote copies, remote signals or barrier semaphores. Data moves between devices by JAX's collectives and lax.ppermute only.
A program may use at most 128 MiB of HBM per device.

```python
import math
import jax
import jax.numpy as jnp
import numpy as np
from jax import lax

D = 2048
FF = 5632
HEADS = 16
KV_HEADS = 8
HD = 64
WINDOW = 128
TOK_DEV = 512
TOKENS = 8192
DOCS = 8
N_TP = 2


def draw_pair(key):
    base = jax.random.fold_in(key, 17)
    first, second = jax.random.split(base, 2)
    queries = jnp.clip(jax.random.normal(first, (TOKENS, HEADS * HD), jnp.float32), -6.0, 6.0)
    keys = jnp.clip(jax.random.normal(second, (TOKENS, KV_HEADS * HD), jnp.float32), -6.0, 6.0)
    return (queries, keys)


def draw_queries(key, part):
    return draw_pair(key)[0].astype(jnp.bfloat16)


def draw_keys(key, part):
    return draw_pair(key)[1].astype(jnp.bfloat16)


def block_scale(stream_key, dims, cuts, low, top_value):
    loudness, own = 1.0, jax.random.fold_in(stream_key, 6)
    for position, shards_of in cuts:
        steps = jnp.exp(jax.random.uniform(jax.random.fold_in(own, position), (shards_of,), jnp.float32, low / len(cuts), top_value / len(cuts)))
        loudness = loudness * jnp.repeat(steps, dims[position] // shards_of).reshape([-1 if axis == position else 1 for axis in range(len(dims))])
    return loudness


def length_profile(amount, total, limit, skew):
    weights = [(1 << 20) // math.isqrt(rank ** skew) + 1 for rank in range(2, amount + 1)]
    surplus, given = total - limit - (amount - 1), [1] * (amount - 1)
    while surplus > 0:
        candidates = [i for i in range(amount - 1) if given[i] < limit]
        pool, remaining = sum([weights[i] for i in candidates]), surplus
        for i in candidates:
            addition = min(limit - given[i], max(1, remaining * weights[i] // pool), surplus)
            given[i] = given[i] + addition
            surplus = surplus - addition
    return np.array([limit] + given)


def uneven_parts(key, count, total, most, skew):
    if count == 2:
        one = jax.random.randint(key, (), max(1, total - most), min(most, total - 1) + 1)
        return jnp.stack([one, total - one])
    tallies = jnp.asarray(length_profile(count, total, most, skew), jnp.int32)
    twos = (count - 1) // 2
    giver, receiver = tallies[1:1 + 2 * twos:2], tallies[2:2 + 2 * twos:2]
    slack = jnp.minimum(giver - 1, most - receiver)
    shifted = jax.random.randint(jax.random.fold_in(key, 1), (twos,), 0, 1 << 20) % (slack + 1)
    tallies = tallies.at[1:1 + 2 * twos:2].set(giver - shifted).at[2:2 + 2 * twos:2].set(receiver + shifted)
    return tallies[jax.random.permutation(jax.random.fold_in(key, 2), count)]


def noise(key, shape, deviation, limit, cuts=(), held_as=jnp.bfloat16):
    loudness = block_scale(key, shape, cuts, -0.22, 0.18) if cuts else 1.0
    entries = jax.random.normal(key, shape, jnp.float32) * deviation * loudness
    return jnp.minimum(jnp.maximum(entries, -limit), limit).astype(held_as)


def setup_inputs(seed: int = 0) -> dict:
    splits = jax.random.split(jax.random.key(seed), 12)
    resid = noise(splits[0], (TOKENS, D), 0.5, 3.0, ((0, 32),))
    queries = draw_queries(jax.random.fold_in(splits[11], 71), 0)
    keys = draw_keys(jax.random.fold_in(splits[11], 71), 0)
    values = noise(splits[3], (TOKENS, KV_HEADS * HD), 1.0, 6.0, ((0, 16), (1, 2)))
    documents = jnp.searchsorted(jnp.cumsum(uneven_parts(splits[4], DOCS, TOKENS, 4 * TOK_DEV, 0)), jnp.arange(TOKENS), side="right").astype(jnp.int32)
    sinks = jnp.clip(5.0 * jax.random.uniform(splits[5], (HEADS,), jnp.float32) ** block_scale(splits[5], (HEADS,), ((0, 2),), -0.2, 0.2), 0.0, 5.0)
    out_proj = noise(splits[6], (HEADS * HD, D), HD ** -0.5, 0.75)
    norm_gain = jnp.clip(1.0 + 0.18 * jax.random.normal(splits[7], (D,), jnp.float32), 0.1, 1.9)
    gate_proj = noise(splits[8], (D, FF), D ** -0.5, 0.125, ((0, 16), (1, 2)))
    up_proj = noise(splits[9], (D, FF), D ** -0.5, 0.125, ((0, 16), (1, 2)))
    down_proj = noise(splits[10], (FF, D), FF ** -0.5, 0.078125, ((0, 2), (1, 16)))
    return {"resid": resid, "queries": queries, "keys": keys, "values": values, "documents": documents, "sinks": sinks, "out_proj": out_proj, "norm_gain": norm_gain, "gate_proj": gate_proj, "up_proj": up_proj, "down_proj": down_proj}


def band_attend(queries, keys, values, documents, sinks):
    rows = queries.shape[0]
    kv_heads = keys.shape[1] // HD
    group = queries.shape[1] // HD // kv_heads
    blocks = rows // WINDOW
    zero_keys = jnp.zeros((WINDOW, keys.shape[1]), jnp.float32)
    ext_keys = jnp.concatenate([zero_keys, keys.astype(jnp.float32)], axis=0).reshape(blocks + 1, WINDOW, kv_heads, HD)
    ext_values = jnp.concatenate([zero_keys, values.astype(jnp.float32)], axis=0).reshape(blocks + 1, WINDOW, kv_heads, HD)
    ext_docs = jnp.concatenate([jnp.zeros((WINDOW,), jnp.int32), documents.astype(jnp.int32)], axis=0).reshape(blocks + 1, WINDOW)
    band_keys = jnp.concatenate([ext_keys[:-1], ext_keys[1:]], axis=1)
    band_values = jnp.concatenate([ext_values[:-1], ext_values[1:]], axis=1)
    band_docs = jnp.concatenate([ext_docs[:-1], ext_docs[1:]], axis=1)
    query_docs = documents.reshape(blocks, WINDOW)
    distance = jnp.arange(WINDOW)[:, None] + WINDOW - jnp.arange(2 * WINDOW)[None, :]
    key_pos = jnp.arange(blocks)[:, None] * WINDOW + jnp.arange(2 * WINDOW)[None, :] - WINDOW
    visible = ((distance >= 0) & (distance < WINDOW))[None] & (key_pos >= 0)[:, None, :] & (band_docs[:, None, :] == query_docs[:, :, None])
    query_blocks = queries.astype(jnp.float32).reshape(blocks, WINDOW, kv_heads, group, HD)
    scores = jnp.einsum('nikgd,njkd->nkgij', query_blocks, band_keys) * HD ** (-0.5)
    scores = jnp.where(visible[:, None, None], scores, -jnp.inf)
    sink_logit = sinks.astype(jnp.float32).reshape(kv_heads, group)[None, :, :, None, None]
    row_top = jnp.maximum(lax.optimization_barrier(jnp.max(scores, axis=-1, keepdims=True)), sink_logit)
    raw_weights = jnp.exp(scores - row_top)
    totals = lax.optimization_barrier(jnp.sum(raw_weights, axis=-1, keepdims=True)) + jnp.exp(sink_logit - row_top)
    weights = (raw_weights / totals).astype(jnp.bfloat16).astype(jnp.float32)
    attended = jnp.einsum('nkgij,njkd->nikgd', weights, band_values)
    return attended.astype(jnp.bfloat16).reshape(rows, kv_heads * group * HD)

def reference(resid, queries, keys, values, documents, sinks, out_proj, norm_gain, gate_proj, up_proj, down_proj):
    group = HEADS // KV_HEADS
    pieces = []
    for head in range(KV_HEADS):
        pieces.append(band_attend(queries[:, head * group * HD:(head + 1) * group * HD], keys[:, head * HD:(head + 1) * HD], values[:, head * HD:(head + 1) * HD], documents, sinks[head * group:(head + 1) * group]))
    attended = jnp.concatenate(pieces, axis=1)
    mid_rows = resid.astype(jnp.float32) + jnp.dot(attended, out_proj, preferred_element_type=jnp.float32)
    scale = lax.rsqrt(lax.optimization_barrier(jnp.mean(mid_rows * mid_rows, axis=-1, keepdims=True)) + 1e-06)
    normed = (mid_rows * scale * norm_gain).astype(jnp.bfloat16)
    width = FF // N_TP

    def ffn_rows(row_block):
        gate_acts = jnp.dot(row_block, gate_proj, preferred_element_type=jnp.float32)
        up_acts = jnp.dot(row_block, up_proj, preferred_element_type=jnp.float32)
        hidden = (jax.nn.silu(gate_acts) * up_acts).astype(jnp.bfloat16)
        totals = jnp.zeros((row_block.shape[0], D), jnp.float32)
        for block in range(N_TP):
            partial_value = jnp.dot(hidden[:, block * width:(block + 1) * width], down_proj[block * width:(block + 1) * width], preferred_element_type=jnp.float32).astype(jnp.bfloat16)
            totals = totals + lax.optimization_barrier(partial_value).astype(jnp.float32)
        return totals
    summed = lax.map(ffn_rows, normed.reshape(TOKENS // TOK_DEV, TOK_DEV, D)).reshape(TOKENS, D)
    return (mid_rows + summed).astype(jnp.bfloat16)
```

```python
from functools import partial

import jax
import jax.numpy as jnp
from jax import lax
from jax.experimental import pallas as pl
from jax.experimental.pallas import tpu as pltpu
from jax.sharding import PartitionSpec as P

HD = 64
WINDOW = 128
LANES = 128
VMEM_BYTES = 56 * 1024 * 1024


def passed_along(value, axis, steps):
    count = lax.axis_size(axis)
    first, last = (max(0, -steps), min(count, count - steps))
    return lax.ppermute(value, axis, [(source, source + steps) for source in range(first, last)])


def swapped(value, axis, mask):
    count = lax.axis_size(axis)
    return lax.ppermute(value, axis, [(source, source ^ mask) for source in range(count)])


def tied(value, *others):
    return lax.optimization_barrier((value, *others))[0]


def attend(queries, keys, values, documents, sinks):
    rows = queries.shape[0]
    kv_heads = keys.shape[1] // HD
    group = queries.shape[1] // HD // kv_heads
    blocks = rows // WINDOW
    key_value = jnp.concatenate([keys, values], axis=1)
    tail_pair, tail_docs = passed_along(
        (key_value[rows - WINDOW :], documents[rows - WINDOW :].astype(jnp.bfloat16)), "sp", 1
    )
    ext_pair = jnp.concatenate([tail_pair, key_value], axis=0).reshape(
        blocks + 1, WINDOW, 2 * kv_heads * HD
    )
    ext_docs = jnp.concatenate([tail_docs.astype(jnp.int32), documents], axis=0).reshape(
        blocks + 1, WINDOW
    )
    band = jnp.concatenate([ext_pair[:-1], ext_pair[1:]], axis=1)
    band_keys = band[:, :, : kv_heads * HD].reshape(blocks, 2 * WINDOW, kv_heads, HD)
    band_values = band[:, :, kv_heads * HD :].reshape(blocks, 2 * WINDOW, kv_heads, HD)
    band_docs = jnp.concatenate([ext_docs[:-1], ext_docs[1:]], axis=1)
    query_docs = documents.reshape(blocks, WINDOW)
    offset = lax.axis_index("sp") * rows
    distance = jnp.arange(WINDOW)[:, None] + WINDOW - jnp.arange(2 * WINDOW)[None, :]
    key_pos = (
        offset + jnp.arange(blocks)[:, None] * WINDOW + jnp.arange(2 * WINDOW)[None, :] - WINDOW
    )
    visible = (
        ((distance >= 0) & (distance < WINDOW))[None]
        & (key_pos >= 0)[:, None, :]
        & (band_docs[:, None, :] == query_docs[:, :, None])
    )
    query_blocks = queries.reshape(blocks, WINDOW, kv_heads, group, HD)
    scores = jnp.einsum(
        "nikgd,njkd->nkgij", query_blocks, band_keys, preferred_element_type=jnp.float32
    ) * HD ** (-0.5)
    scores = jnp.where(visible[:, None, None], scores, -jnp.inf)
    sink_logit = sinks.reshape(kv_heads, group)[None, :, :, None, None]
    row_top = jnp.maximum(jnp.max(scores, axis=-1, keepdims=True), sink_logit)
    raw_weights = jnp.exp(scores - row_top)
    totals = jnp.sum(raw_weights, axis=-1, keepdims=True) + jnp.exp(sink_logit - row_top)
    weights = (raw_weights / totals).astype(jnp.bfloat16)
    attended = jnp.einsum(
        "nkgij,njkd->nikgd", weights, band_values, preferred_element_type=jnp.float32
    )
    return attended.astype(jnp.bfloat16).reshape(rows, kv_heads * group * HD)


def norm_rows(mid_rows, norm_gain):
    scale = lax.rsqrt(jnp.mean(mid_rows * mid_rows, axis=-1, keepdims=True) + 1e-06)
    return (mid_rows * scale * norm_gain).astype(jnp.bfloat16)


def gathered_cols(slot_ref, row_refs, out_ref, count):
    rows = row_refs[0].shape[0]
    for piece, ref in enumerate(row_refs):
        for at in range(count):
            start = pl.multiple_of(slot_ref[at] * LANES, LANES)
            out_ref[piece * rows : (piece + 1) * rows, at * LANES : (at + 1) * LANES] = ref[
                :, pl.ds(start, LANES)
            ]


def gate_up_body(count, has_acc, last, slot_ref, *refs):
    row_refs, refs = refs[:4], refs[4:]
    gate_refs, refs = refs[:count], refs[count:]
    up_refs, refs = refs[:count], refs[count:]
    if has_acc:
        acc_ref, refs = refs[0], refs[1:]
    out_ref, cols_ref = refs

    @pl.when(pl.program_id(0) == 0)
    def _():
        gathered_cols(slot_ref, row_refs, cols_ref, count)

    pair = jnp.concatenate(
        [
            jnp.concatenate([gate[...], up[...]], axis=1)
            for gate, up in zip(gate_refs, up_refs)
        ],
        axis=0,
    )
    acts = jnp.dot(cols_ref[...], pair, preferred_element_type=jnp.float32)
    if has_acc:
        acts = acts + acc_ref[...]
    if last:
        gate_acts, up_acts = acts[:, :LANES], acts[:, LANES:]
        hidden = gate_acts / (1.0 + jnp.exp(-gate_acts)) * up_acts
        out_ref[...] = hidden.astype(out_ref.dtype)
    else:
        out_ref[...] = acts


def gate_up(slots, row_pieces, slices, acc=None, last=False):
    count = len(slices)
    rows, width = row_pieces[0].shape
    total = rows * len(row_pieces)
    depth, both = slices[0].shape
    tiles = both // 2 // LANES
    whole = pl.BlockSpec((rows, width), lambda n, s: (0, 0))
    in_specs = (
        [whole] * len(row_pieces)
        + [pl.BlockSpec((depth, LANES), lambda n, s: (0, n))] * count
        + [pl.BlockSpec((depth, LANES), lambda n, s: (0, n + tiles))] * count
    )
    args = list(row_pieces) + list(slices) * 2
    if acc is not None:
        in_specs.append(pl.BlockSpec((total, 2 * LANES), lambda n, s: (0, n)))
        args.append(acc)
    if last:
        out_shape = jax.ShapeDtypeStruct((total, both // 2), jnp.bfloat16)
        out_spec = pl.BlockSpec((total, LANES), lambda n, s: (0, n))
    else:
        out_shape = jax.ShapeDtypeStruct((total, both), jnp.float32)
        out_spec = pl.BlockSpec((total, 2 * LANES), lambda n, s: (0, n))
    flops = 2 * total * count * depth * both
    return pl.pallas_call(
        partial(gate_up_body, count, acc is not None, last),
        out_shape=out_shape,
        grid_spec=pltpu.PrefetchScalarGridSpec(
            num_scalar_prefetch=1,
            grid=(tiles,),
            in_specs=in_specs,
            out_specs=out_spec,
            scratch_shapes=[pltpu.VMEM((total, count * LANES), jnp.bfloat16)],
        ),
        compiler_params=pltpu.CompilerParams(vmem_limit_bytes=VMEM_BYTES),
        cost_estimate=pl.CostEstimate(
            flops=flops, transcendentals=0, bytes_accessed=total * both * 4
        ),
        name="gate_up_last" if last else "gate_up",
    )(slots, *args)


def down_body(count, hidden_ref, *refs):
    slice_refs, (send_ref, keep_ref) = refs[:count], refs[count:]
    weights = jnp.concatenate([ref[...] for ref in slice_refs], axis=1)
    partial_rows = jnp.dot(hidden_ref[...], weights, preferred_element_type=jnp.float32).astype(
        jnp.bfloat16
    )
    step = pl.program_id(0)

    @pl.when(step < 2)
    def _():
        send_ref[...] = partial_rows

    @pl.when(step >= 2)
    def _():
        keep_ref[...] = partial_rows


def down(hidden, slices, order):
    count = len(slices)
    rows = hidden.shape[0] // 4
    depth, lanes = slices[0].shape
    width = count * lanes

    def piece(step, *_):
        where = jnp.int32(order[0])
        for at in range(1, 4):
            where = jnp.where(step == at, jnp.int32(order[at]), where)
        return (where, 0)

    shape = jax.ShapeDtypeStruct((2 * rows, width), jnp.bfloat16)
    return pl.pallas_call(
        partial(down_body, count),
        out_shape=(shape, shape),
        grid=(4,),
        in_specs=[pl.BlockSpec((rows, depth), piece)]
        + [pl.BlockSpec((depth, lanes), lambda n: (0, 0))] * count,
        out_specs=(
            pl.BlockSpec((rows, width), lambda n: (jnp.minimum(n, 1), 0)),
            pl.BlockSpec((rows, width), lambda n: (jnp.maximum(n - 2, 0), 0)),
        ),
        compiler_params=pltpu.CompilerParams(vmem_limit_bytes=VMEM_BYTES),
        cost_estimate=pl.CostEstimate(
            flops=2 * 4 * rows * depth * width, transcendentals=0, bytes_accessed=4 * rows * depth
        ),
        name="down",
    )(hidden, *slices)


def finish_body(count, slot_ref, mid_ref, *refs):
    own_refs, other_refs, out_ref = refs[: count // 4], refs[count // 4 : -1], refs[-1]
    for at in range(count):
        start = pl.multiple_of(slot_ref[at] * LANES, LANES)
        inside = slice(at % 4 * LANES, (at % 4 + 1) * LANES)
        summed = own_refs[at // 4][:, inside] + other_refs[at // 4][:, inside].astype(jnp.float32)
        out_ref[:, pl.ds(start, LANES)] = (mid_ref[:, pl.ds(start, LANES)] + summed).astype(
            out_ref.dtype
        )


def finish(slots, mid_rows, own, other):
    vmem = pl.BlockSpec(memory_space=pltpu.VMEM)
    return pl.pallas_call(
        partial(finish_body, slots.shape[0]),
        out_shape=jax.ShapeDtypeStruct(mid_rows.shape, jnp.bfloat16),
        in_specs=[pl.BlockSpec(memory_space=pltpu.SMEM)]
        + [vmem] * (1 + len(own) + len(other)),
        out_specs=vmem,
        compiler_params=pltpu.CompilerParams(vmem_limit_bytes=VMEM_BYTES),
        name="finish",
    )(slots, mid_rows, *own, *other)


def exchanged(
    resid,
    queries,
    keys,
    values,
    documents,
    sinks,
    out_proj,
    norm_gain,
    gate_proj,
    up_proj,
    down_proj,
):
    sp, tp = lax.axis_index("sp"), lax.axis_index("tp")
    count = lax.axis_size("sp")
    stages = count // 4
    half = gate_proj.shape[1] // 2
    part = (sp // 4) % 2

    def gate_up_of(which):
        return jnp.concatenate(
            [lax.dynamic_slice_in_dim(w, which * half, half, axis=1) for w in (gate_proj, up_proj)],
            axis=1,
        )

    def down_of(which):
        return lax.dynamic_slice_in_dim(down_proj, which * half, half, axis=0)

    gu_same, gu_diff = gate_up_of(part), gate_up_of(1 - part)
    gu = [gu_same, swapped(gu_diff, "sp", 4), swapped(gu_same, "sp", 8), None]
    attended = attend(queries, keys, values, documents, sinks)
    rows = attended.shape[0] // 2
    sent = lax.dynamic_slice_in_dim(attended, (1 - tp) * rows, rows, axis=0)
    kept = lax.dynamic_slice_in_dim(attended, tp * rows, rows, axis=0)
    came = swapped(sent, "tp", 1)
    width = attended.shape[1]
    mid_rows = (
        resid.astype(jnp.float32)
        + jnp.dot(
            kept,
            lax.dynamic_slice_in_dim(out_proj, tp * width, width, axis=0),
            preferred_element_type=jnp.float32,
        )
        + jnp.dot(
            came,
            lax.dynamic_slice_in_dim(out_proj, (1 - tp) * width, width, axis=0),
            preferred_element_type=jnp.float32,
        )
    )
    normed = norm_rows(mid_rows, norm_gain)
    normed_z = swapped(normed, "sp", 4)
    normed_x = swapped(normed, "tp", 1)
    normed_xz = swapped(normed_z, "tp", 1)
    pieces = [normed, normed_x, normed_z, normed_xz]
    gu[3] = swapped(tied(gu_diff, normed), "sp", 12)
    down_same, down_diff = down_of(part), down_of(1 - part)
    down_same, down_diff = tied(down_same, normed), tied(down_diff, normed)
    dn = [
        down_same,
        swapped(down_diff, "sp", 4),
        swapped(down_same, "sp", 8),
        swapped(down_diff, "sp", 12),
    ]

    def spread(piece):
        across = swapped(piece, "sp", 2)
        return [piece, swapped(piece, "sp", 1), across, swapped(across, "sp", 1)]

    slots = jnp.bitwise_xor(sp, jnp.arange(count, dtype=jnp.int32))
    gu_all = [spread(piece) for piece in gu]
    acc = gate_up(slots[:12], pieces, gu_all[0] + gu_all[1] + gu_all[2])
    hidden = gate_up(slots[12:], pieces, gu_all[3], acc, last=True)
    own, other = [None] * stages, [None] * stages
    keeps, comes = [], []
    for stage in range(stages):
        x_first = stage >= 2
        send, keep = down(hidden, spread(dn[stage]), (1, 3, 0, 2) if x_first else (2, 3, 0, 1))
        keeps.append(keep)
        comes.append(swapped(send, "tp", 1) if x_first else swapped(send, "sp", 4))
    for stage in range(stages):
        x_first = stage >= 2
        got = comes[stage if x_first else stage ^ 1]
        summed = keeps[stage].astype(jnp.float32) + got.astype(jnp.float32)
        own[stage] = summed[:rows]
        second = summed[rows:].astype(jnp.bfloat16)
        if x_first:
            other[stage ^ 1] = swapped(second, "sp", 4)
        else:
            other[stage] = swapped(second, "tp", 1)
    return finish(slots, mid_rows, own, other)


def gathered(
    resid,
    queries,
    keys,
    values,
    documents,
    sinks,
    out_proj,
    norm_gain,
    gate_proj,
    up_proj,
    down_proj,
):
    attended = attend(queries, keys, values, documents, sinks)
    own_heads = lax.all_to_all(attended, "tp", split_axis=0, concat_axis=1, tiled=True)
    mid_rows = resid.astype(jnp.float32) + jnp.dot(
        own_heads, out_proj, preferred_element_type=jnp.float32
    )
    normed = lax.all_gather(norm_rows(mid_rows, norm_gain), "tp", axis=0, tiled=True)
    gate_acts = jnp.dot(
        normed,
        lax.all_gather(gate_proj, "sp", axis=0, tiled=True),
        preferred_element_type=jnp.float32,
    )
    up_acts = jnp.dot(
        normed,
        lax.all_gather(up_proj, "sp", axis=0, tiled=True),
        preferred_element_type=jnp.float32,
    )
    down_local = lax.all_gather(down_proj, "sp", axis=1, tiled=True)
    hidden = (jax.nn.silu(gate_acts) * up_acts).astype(jnp.bfloat16)
    summed = lax.psum_scatter(
        jnp.dot(hidden, down_local, preferred_element_type=jnp.float32).astype(jnp.bfloat16),
        "tp",
        scatter_dimension=0,
        tiled=True,
    ).astype(jnp.float32)
    return (mid_rows + summed).astype(jnp.bfloat16)


def solution(mesh):
    in_specs = (
        P(("sp", "tp"), None),
        P("sp", "tp"),
        P("sp", "tp"),
        P("sp", "tp"),
        P("sp"),
        P("tp"),
        P(),
        P(),
        P("sp", "tp"),
        P("sp", "tp"),
        P("tp", "sp"),
    )
    out_specs = P(("sp", "tp"), None)
    small = mesh.shape["tp"] == 2 and mesh.shape["sp"] == 16
    return jax.shard_map(
        exchanged if small else gathered,
        mesh=mesh,
        in_specs=in_specs,
        out_specs=out_specs,
        check_vma=False,
    )
```
